32 devices in a mesh: sp: 16 (over z, y, core), tp: 2 (over x).
Axes of the slice: x: 2, y: 2, z: 4, core: 2. Of those that a mesh axis runs over, the one named last changes fastest.
Arguments:
- tokens: bfloat16 [6144, 2048], P('sp', 'tp'), may hold values from -60 to 60
- pre_gain: bfloat16 [2048], P('tp'), may hold values from 0.099609375 to 1.8984375
- w_query: bfloat16 [2048, 1024], P('sp', 'tp'), may hold values from -1 to 1
- w_key: bfloat16 [2048, 1024], P('sp', 'tp'), may hold values from -1 to 1
- w_value: bfloat16 [2048, 1024], P('sp', 'tp'), may hold values from -0.125 to 0.125
- w_pool: bfloat16 [2048, 1024], P('sp', 'tp'), may hold values from -0.125 to 0.125
- lambdas: float32 [8], P('tp'), may hold values from 0.3 to 0.8
- sub_gain: float32 [128], replicated, may hold values from 0.1 to 1.9
- group_weight: bfloat16 [8, 128, 128], P('tp'), may hold values from -0.5 to 0.5
- pool_scale: float32 [1024], P('tp'), may hold values from 0.1 to 1.9
- w_out: bfloat16 [2048, 2048], P('tp', 'sp'), may hold values from -0.125 to 0.125
Outputs:
- mixed_out: bfloat16 [6144, 2048], P(('sp', 'tp'))
The draws below stay inside these ranges and needn't reach their ends.
All inputs are finite; a program needn't handle non-finite values.
Results may differ from the reference program's by a relative error of at most 0.015.
Values may be sent and summed in bfloat16 or wider, within the bound.
No kernel may reach another device: no remote copies, remote signals or barrier semaphores. Data moves between devices by JAX's collectives and lax.ppermute only.
A program may use at most 128 MiB of HBM per device.

```python
import math
import jax
import jax.numpy as jnp
import numpy as np
from jax import lax

D = 2048
HEADS = 8
HDIM = 64
VDIM = 128
GROUPS = 8
GDIM = 128
TOKENS = 6144


def draw_tokens(key, part):
    noise = jax.random.normal(jax.random.fold_in(key, 11), (TOKENS, D), jnp.float32)
    row_scale = jnp.exp(jax.random.uniform(jax.random.fold_in(key, 12), (TOKENS, 1), jnp.float32, 0.0, math.log(10.0)))
    column_rise = 1.1 * jnp.arange(D, dtype=jnp.float32)[None, :] / D
    column_scale = jnp.exp(jax.random.uniform(jax.random.fold_in(key, 13), (1, D), jnp.float32, -0.7, 0.7) + column_rise)
    result = noise * row_scale * column_scale
    return jnp.clip(result, -60.0, 60.0).astype(jnp.bfloat16)


def query_key_pair(key):
    columns = HEADS * 2 * HDIM
    spread = math.sqrt(2.0 / D)
    first = jax.random.normal(jax.random.fold_in(key, 21), (D, columns), jnp.float32) * spread
    second = jax.random.normal(jax.random.fold_in(key, 22), (D, columns), jnp.float32) * spread
    return (jnp.clip(first, -1.0, 1.0), jnp.clip(second, -1.0, 1.0))


def draw_w_query(key, part):
    return query_key_pair(key)[0].astype(jnp.bfloat16)


def draw_w_key(key, part):
    return query_key_pair(key)[1].astype(jnp.bfloat16)


def level_of(rng, shape, split, least, high):
    factor_of, own = 1.0, jax.random.fold_in(rng, 6)
    for dim, shards_of in split:
        heights = jnp.exp(jax.random.uniform(jax.random.fold_in(own, dim), (shards_of,), jnp.float32, least / len(split), high / len(split)))
        factor_of = factor_of * jnp.repeat(heights, shape[dim] // shards_of).reshape([-1 if axis == dim else 1 for axis in range(len(shape))])
    return factor_of


def bell_draw(stream_key, extent, width, reach, shards=(), held_as=jnp.bfloat16):
    values = jax.random.normal(stream_key, extent, jnp.float32) * width
    if len(shards) > 0:
        values = level_of(stream_key, extent, shards, -0.22, 0.18) * values
    return jnp.clip(values, min=-reach, max=reach).astype(held_as)


def setup_inputs(seed: int = 0) -> dict:
    splits = jax.random.split(jax.random.key(seed), 12)
    tokens = draw_tokens(jax.random.fold_in(splits[11], 71), 0)
    pre_gain = jnp.clip(1.0 + 0.18 * jax.random.normal(splits[1], (D,), jnp.float32), 0.099609375, 1.8984375).astype(jnp.bfloat16)
    w_query = draw_w_query(jax.random.fold_in(splits[11], 71), 0)
    w_key = draw_w_key(jax.random.fold_in(splits[11], 71), 0)
    w_value = bell_draw(splits[4], (D, HEADS * VDIM), D ** -0.5, 0.125, ((0, 16), (1, 2)))
    w_pool = bell_draw(splits[5], (D, GROUPS * GDIM), D ** -0.5, 0.125, ((0, 16), (1, 2)))
    lambdas = jnp.clip(0.3 + 0.5 * jax.random.uniform(splits[6], (HEADS,), jnp.float32) ** level_of(splits[6], (HEADS,), ((0, 2),), -0.2, 0.2), 0.3, 0.8)
    sub_gain = jnp.clip(1.0 + 0.18 * jax.random.normal(splits[7], (VDIM,), jnp.float32), 0.1, 1.9)
    group_weight = bell_draw(splits[8], (GROUPS, GDIM, GDIM), GDIM ** -0.5, 0.5, ((0, 2),))
    pool_scale = jnp.clip(1.0 + 0.18 * jax.random.normal(splits[9], (GROUPS * GDIM,), jnp.float32), 0.1, 1.9)
    w_out = bell_draw(splits[10], (HEADS * (VDIM + GDIM), D), (HEADS * (VDIM + GDIM)) ** -0.5, 0.125, ((0, 2), (1, 16)))
    return {"tokens": tokens, "pre_gain": pre_gain, "w_query": w_query, "w_key": w_key, "w_value": w_value, "w_pool": w_pool, "lambdas": lambdas, "sub_gain": sub_gain, "group_weight": group_weight, "pool_scale": pool_scale, "w_out": w_out}


EPSILON = 1e-06
WINDOWS = (2, 4, 8, 16)
RIM_ROWS = 15

def head_block(query_head, key_head, value_head, weight_two, first_row):
    block_len = query_head.shape[0]
    key_len = key_head.shape[0]
    score_scale = 1.0 / math.sqrt(HDIM)
    scores = jnp.einsum('qmd,kmd->mqk', query_head.astype(jnp.float32), key_head.astype(jnp.float32)) * score_scale
    allowed = jnp.arange(key_len, dtype=jnp.int32)[None, :] <= (first_row + jnp.arange(block_len, dtype=jnp.int32))[:, None]
    scores = jnp.where(allowed[None], scores, -jnp.inf)
    row_max = lax.optimization_barrier(jnp.max(scores, axis=-1, keepdims=True))
    expo = jnp.where(allowed[None], jnp.exp(scores - row_max), 0.0)
    row_sum = lax.optimization_barrier(jnp.sum(expo, axis=-1))
    rounded = lax.optimization_barrier(expo.astype(jnp.bfloat16)).astype(jnp.float32)
    weighted = jnp.einsum('mqk,kd->mqd', rounded, value_head.astype(jnp.float32))
    head_mix = weighted[0] / row_sum[0][:, None] - weight_two * weighted[1] / row_sum[1][:, None]
    return head_mix

def reference(tokens, pre_gain, w_query, w_key, w_value, w_pool, lambdas, sub_gain, group_weight, pool_scale, w_out):
    features = tokens.astype(jnp.float32)
    inverse = lax.rsqrt(lax.optimization_barrier(jnp.mean(features * features, axis=1, keepdims=True)) + EPSILON)
    scaled = (features * pre_gain.astype(jnp.float32)).astype(jnp.bfloat16)

    def project(weight):
        return (jnp.dot(scaled, weight, preferred_element_type=jnp.float32) * inverse).astype(jnp.bfloat16)
    queries = project(w_query).reshape(TOKENS, HEADS, 2, HDIM)
    key_rows = project(w_key).reshape(TOKENS, HEADS, 2, HDIM)
    values = project(w_value).reshape(TOKENS, HEADS, VDIM)
    pool_in = project(w_pool)
    block_len = math.gcd(TOKENS, 512)
    pieces = []
    for block_index in range(TOKENS // block_len):
        first_row = block_index * block_len
        key_len = first_row + block_len
        query_heads = jnp.transpose(queries[first_row:key_len], (1, 0, 2, 3))
        key_heads = jnp.transpose(key_rows[:key_len], (1, 0, 2, 3))
        value_heads = jnp.transpose(values[:key_len], (1, 0, 2))

        def one_head(packed):
            return head_block(packed[0], packed[1], packed[2], packed[3], first_row)
        mixed_heads = lax.map(one_head, (query_heads, key_heads, value_heads, lambdas))
        mean_sq = lax.optimization_barrier(jnp.mean(mixed_heads * mixed_heads, axis=-1, keepdims=True))
        normed = mixed_heads * lax.rsqrt(mean_sq + EPSILON) * sub_gain
        pieces.append(jnp.transpose(normed, (1, 0, 2)).astype(jnp.bfloat16))
    attention = jnp.concatenate(pieces, axis=0)
    pool_float = pool_in.astype(jnp.float32)
    extended = jnp.concatenate([jnp.zeros((RIM_ROWS, GROUPS * GDIM), jnp.float32), pool_float], axis=0)
    running = jnp.concatenate([jnp.zeros((1, GROUPS * GDIM), jnp.float32), jnp.cumsum(extended, axis=0)], axis=0)
    running_top = running[RIM_ROWS + 1:]
    positions = jnp.arange(TOKENS, dtype=jnp.int32)
    window_of_column = np.repeat(np.arange(GROUPS) % len(WINDOWS), GDIM)
    average = jnp.zeros_like(running_top)
    for window_slot, window_span in enumerate(WINDOWS):
        running_low = running[RIM_ROWS + 1 - window_span:RIM_ROWS + 1 - window_span + TOKENS]
        window_count = jnp.minimum(positions + 1, window_span).astype(jnp.float32)
        average = average + jnp.where(window_of_column[None, :] == window_slot, (running_top - running_low) / window_count[:, None], 0.0)
    differ = (average - pool_float).astype(jnp.bfloat16).reshape(TOKENS, GROUPS, GDIM)
    pooled = jnp.einsum('tgc,gcd->tgd', differ.astype(jnp.float32), group_weight.astype(jnp.float32))
    pooled = (pooled * pool_scale.reshape(GROUPS, GDIM)).astype(jnp.bfloat16)
    branch = jnp.concatenate([attention, pooled], axis=2).reshape(TOKENS, HEADS * (VDIM + GDIM))
    return jnp.dot(branch, w_out, preferred_element_type=jnp.float32).astype(jnp.bfloat16)
```

```python
import functools
import math

import jax
import jax.numpy as jnp
from jax import lax
from jax.experimental import pallas as pl
from jax.experimental.pallas import tpu as pltpu
from jax.sharding import PartitionSpec as P

EPSILON = 1e-06
NEG_LARGE = -1e30
WINDOWS = (2, 4, 8, 16)
RIM_ROWS = 15


def passed_along(block, axis, distance):
    devices = range(lax.axis_size(axis))
    route = [(i - distance, i) for i in devices if i - distance in devices]
    return lax.ppermute(block, axis, route)


def swapped(block, axis):
    return lax.ppermute(block, axis, [(0, 1), (1, 0)])


def attention_kernel(
    place_ref, lam_ref, gain_ref, q_ref, kv_ref, out_ref, max_ref, acc_ref, *, inner, head_dim
):
    rows = q_ref.shape[2]
    value_dim = out_ref.shape[3]
    pair = 2 * head_dim
    scale = math.log2(math.e) / math.sqrt(head_dim)
    query_block = pl.program_id(1) * inner + place_ref[0]
    query = q_ref[0, 0]
    lane = lax.broadcasted_iota(jnp.int32, (rows, pair), 1)
    blank = jnp.zeros_like(query)
    both = jnp.concatenate(
        [jnp.where(lane < head_dim, query, blank), jnp.where(lane < head_dim, blank, query)], axis=0
    )
    ones = jnp.ones((rows, value_dim), jnp.bfloat16)

    def scores_of(block):
        keys = kv_ref[block % inner, block // inner, 0, :, :pair]
        return scale * lax.dot_general(
            both, keys, (((1,), (1,)), ((), ())), preferred_element_type=jnp.float32
        )

    def weighted_of(block, expo):
        values = kv_ref[block % inner, block // inner, 0, :, pair:]
        return jnp.dot(
            expo.astype(jnp.bfloat16),
            jnp.concatenate([values, ones], axis=1),
            preferred_element_type=jnp.float32,
        )

    scores = scores_of(query_block)
    row = lax.broadcasted_iota(jnp.int32, scores.shape, 0)
    column = lax.broadcasted_iota(jnp.int32, scores.shape, 1)
    row = jnp.where(row >= rows, row - rows, row)
    scores = jnp.where(column <= row, scores, NEG_LARGE)
    first_max = jnp.max(scores, axis=1, keepdims=True)
    max_ref[...] = jnp.broadcast_to(first_max, max_ref.shape)
    acc_ref[...] = weighted_of(query_block, jnp.exp2(scores - first_max))

    def step(block, carry):
        scores = scores_of(block)
        old_max = max_ref[:, :1]
        new_max = jnp.maximum(old_max, jnp.max(scores, axis=1, keepdims=True))
        expo = jnp.exp2(scores - new_max)
        max_ref[...] = jnp.broadcast_to(new_max, max_ref.shape)
        acc_ref[...] = acc_ref[...] * jnp.exp2(old_max - new_max) + weighted_of(block, expo)
        return carry

    lax.fori_loop(0, query_block, step, 0)
    head_mix = (
        acc_ref[:rows, :value_dim] / acc_ref[:rows, value_dim:]
        - lam_ref[pl.program_id(0)]
        * acc_ref[rows:, :value_dim]
        / acc_ref[rows:, value_dim:]
    )
    mean_sq = jnp.mean(head_mix * head_mix, axis=1, keepdims=True)
    normed = head_mix * lax.rsqrt(mean_sq + EPSILON) * gain_ref[...]
    out_ref[0, 0] = normed.astype(jnp.bfloat16)


def attend(place, lam, gain, queries, kv, head_dim):
    spread, heads, rows, _ = queries.shape
    inner = kv.shape[0]
    value_dim = kv.shape[4] - 2 * head_dim
    smem = pl.BlockSpec(memory_space=pltpu.SMEM)
    return pl.pallas_call(
        functools.partial(attention_kernel, inner=inner, head_dim=head_dim),
        grid=(heads, spread),
        in_specs=[
            smem,
            smem,
            pl.BlockSpec((1, value_dim), lambda h, j: (0, 0)),
            pl.BlockSpec((1, 1, rows, 2 * head_dim), lambda h, j: (j, h, 0, 0)),
            pl.BlockSpec((inner, spread, 1, rows, kv.shape[4]), lambda h, j: (0, 0, h, 0, 0)),
        ],
        out_specs=pl.BlockSpec((1, 1, rows, value_dim), lambda h, j: (j, h, 0, 0)),
        out_shape=jax.ShapeDtypeStruct((spread, heads, rows, value_dim), jnp.bfloat16),
        scratch_shapes=[
            pltpu.VMEM((2 * rows, 128), jnp.float32),
            pltpu.VMEM((2 * rows, 2 * value_dim), jnp.float32),
        ],
        compiler_params=pltpu.CompilerParams(
            dimension_semantics=("arbitrary", "arbitrary"), vmem_limit_bytes=56 << 20
        ),
        cost_estimate=pl.CostEstimate(
            flops=spread * heads * rows * rows * inner * spread * 1024,
            transcendentals=spread * heads * rows * rows * inner * spread,
            bytes_accessed=kv.size * 2,
        ),
        name="diff_attention",
    )(place, lam, gain, queries, kv)


def exchanged(blocks, groups):
    return lax.all_to_all(
        blocks, "sp", split_axis=0, concat_axis=0, tiled=True, axis_index_groups=groups
    )


def local(
    tokens,
    pre_gain,
    w_query,
    w_key,
    w_value,
    w_pool,
    lambdas,
    sub_gain,
    group_weight,
    pool_scale,
    w_out,
):
    tok_rows = tokens.shape[0]
    model_width = tokens.shape[1] * lax.axis_size("tp")
    local_heads = lambdas.shape[0]
    head_dim = w_query.shape[1] // (2 * local_heads)
    value_dim = w_value.shape[1] // local_heads
    local_groups = group_weight.shape[0]
    group_dim = group_weight.shape[1]
    q_cols = w_query.shape[1]
    v_cols = w_value.shape[1]
    sp_size = lax.axis_size("sp")
    tp_size = lax.axis_size("tp")
    spread = math.gcd(local_heads, sp_size)
    inner = sp_size // spread
    heads_here = local_heads // spread
    apart = [[r + inner * j for j in range(spread)] for r in range(inner)]
    beside = [[r + inner * j for r in range(inner)] for j in range(spread)]
    my_sp = lax.axis_index("sp")
    my_tp = lax.axis_index("tp")
    w_cat = jnp.concatenate([w_query, w_key, w_value, w_pool], axis=1)
    w_in_full = lax.all_gather(w_cat, "sp", axis=0, tiled=True)
    gain_row = pre_gain.reshape(1, -1)
    if tp_size == 2:
        other = swapped(tokens, "tp")
        pieces = jnp.where(
            my_tp == 0,
            jnp.concatenate([tokens, other], axis=1),
            jnp.concatenate([other, tokens], axis=1),
        )
    else:
        pieces = lax.all_gather(tokens, "tp", axis=1, tiled=True)
    gains = lax.all_gather(gain_row, "tp", axis=1, tiled=True)
    feature_part = pieces.astype(jnp.float32)
    scaled = (feature_part * gains.astype(jnp.float32)).astype(jnp.bfloat16)
    squares = jnp.sum(feature_part * feature_part, axis=1)
    inverse = lax.rsqrt(squares / model_width + EPSILON)
    projection = jnp.dot(scaled, w_in_full, preferred_element_type=jnp.float32)
    projected = (projection * inverse[:, None]).astype(jnp.bfloat16)
    pair = 2 * head_dim
    queries = jnp.stack([projected[:, h * pair : (h + 1) * pair] for h in range(local_heads)])
    kv = jnp.stack(
        [
            jnp.concatenate(
                [
                    projected[:, q_cols + h * pair : q_cols + (h + 1) * pair],
                    projected[:, 2 * q_cols + h * value_dim : 2 * q_cols + (h + 1) * value_dim],
                ],
                axis=1,
            )
            for h in range(local_heads)
        ]
    )
    pool_in = projected[:, 2 * q_cols + v_cols :]
    positions = my_sp * tok_rows + jnp.arange(tok_rows, dtype=jnp.int32)
    if spread > 1:
        kv = exchanged(kv, apart)
        queries = exchanged(queries, apart)
    kv = kv.reshape(-1, kv.shape[2])
    kv = lax.all_gather(kv, "sp", axis=0, tiled=True, axis_index_groups=beside)
    kv = kv.reshape(inner, spread, heads_here, tok_rows, pair + value_dim)
    queries = queries.reshape(spread, heads_here, tok_rows, pair)
    lam = lax.dynamic_slice_in_dim(lambdas, (my_sp // inner) * heads_here, heads_here)
    place = (my_sp % inner).astype(jnp.int32).reshape(1)
    attention = attend(place, lam, sub_gain.reshape(1, -1), queries, kv, head_dim)
    attention = attention.reshape(local_heads, tok_rows, value_dim)
    if spread > 1:
        attention = exchanged(attention, apart)
    attention = jnp.transpose(attention, (1, 0, 2))
    halo_rows = passed_along(pool_in[tok_rows - RIM_ROWS :], "sp", 1)
    extended = jnp.concatenate([halo_rows, pool_in], axis=0).astype(jnp.float32)
    running = jnp.concatenate(
        [jnp.zeros((1, extended.shape[1]), jnp.float32), jnp.cumsum(extended, axis=0)], axis=0
    )
    running_top = running[RIM_ROWS + 1 :]
    window_ids = (
        lax.axis_index("tp") * local_groups + jnp.arange(local_groups, dtype=jnp.int32)
    ) % len(WINDOWS)
    column_window = jnp.repeat(window_ids, group_dim)
    average = jnp.zeros_like(running_top)
    for window_slot, window_span in enumerate(WINDOWS):
        running_low = running[RIM_ROWS + 1 - window_span : RIM_ROWS + 1 - window_span + tok_rows]
        window_count = jnp.minimum(positions + 1, window_span).astype(jnp.float32)
        average = average + jnp.where(
            column_window[None, :] == window_slot,
            (running_top - running_low) / window_count[:, None],
            0.0,
        )
    differ = (
        (average - pool_in.astype(jnp.float32))
        .astype(jnp.bfloat16)
        .reshape(tok_rows, local_groups, group_dim)
    )
    pooled = jnp.einsum("tgc,gcd->tgd", differ, group_weight, preferred_element_type=jnp.float32)
    pooled = (pooled * pool_scale.reshape(local_groups, group_dim)).astype(jnp.bfloat16)
    branch = jnp.concatenate([attention, pooled], axis=2).reshape(tok_rows, -1)
    w_out_t = lax.all_gather(w_out.T, "sp", axis=0, tiled=True)

    def out_of(rows):
        return lax.dot_general(
            rows, w_out_t, (((1,), (1,)), ((), ())), preferred_element_type=jnp.float32
        )

    if tp_size == 2:
        half = tok_rows // 2
        sent = out_of(lax.dynamic_slice_in_dim(branch, (1 - my_tp) * half, half))
        arrived = swapped(sent.astype(jnp.bfloat16), "tp")
        kept = out_of(lax.dynamic_slice_in_dim(branch, my_tp * half, half))
        return (kept + arrived.astype(jnp.float32)).astype(jnp.bfloat16)
    return lax.psum_scatter(
        out_of(branch).astype(jnp.bfloat16), "tp", scatter_dimension=0, tiled=True
    )


def solution(mesh):
    placed = (
        P("sp", "tp"),
        P("tp"),
        P("sp", "tp"),
        P("sp", "tp"),
        P("sp", "tp"),
        P("sp", "tp"),
        P("tp"),
        P(),
        P("tp", None, None),
        P("tp"),
        P("tp", "sp"),
    )
    return jax.shard_map(
        local, mesh=mesh, in_specs=placed, out_specs=P(("sp", "tp"), None), check_vma=False
    )
```

```python
import functools
import math

import jax
import jax.numpy as jnp
from jax import lax
from jax.experimental import pallas as pl
from jax.experimental.pallas import tpu as pltpu
from jax.sharding import PartitionSpec as P

EPSILON = 1e-06
NEG_LARGE = -1e30
WINDOWS = (2, 4, 8, 16)
RIM_ROWS = 15


def passed_along(block, axis, distance):
    devices = range(lax.axis_size(axis))
    route = [(i - distance, i) for i in devices if i - distance in devices]
    return lax.ppermute(block, axis, route)


def swapped(block, axis):
    return lax.ppermute(block, axis, [(0, 1), (1, 0)])


def attention_kernel(place_ref, lam_ref, gain_ref, q_ref, *refs, inner, head_dim, parts):
    key_refs = refs[:parts]
    value_refs = refs[parts : 2 * parts]
    out_ref, both_ref, max_ref, acc_ref = refs[2 * parts :]
    rows = q_ref.shape[2]
    value_dim = out_ref.shape[3]
    pair = 2 * head_dim
    step_rows = math.gcd(rows, 128)
    scale = math.log2(math.e) / math.sqrt(head_dim)
    mine = place_ref[0]
    query_block = pl.program_id(1) * inner + mine
    query = q_ref[0, 0]
    lane = lax.broadcasted_iota(jnp.int32, (rows, pair), 1)
    blank = jnp.zeros_like(query)
    both_ref[:rows] = jnp.where(lane < head_dim, query, blank)
    both_ref[rows:] = jnp.where(lane < head_dim, blank, query)
    ones = jnp.ones((parts * rows, value_dim), jnp.bfloat16)

    def masked(scores, start, group):
        pieces = []
        for part in range(parts):
            block = group * parts + ((mine ^ part) if parts > 1 else 0)
            piece = scores[:, part * rows : (part + 1) * rows]
            row = lax.broadcasted_iota(jnp.int32, piece.shape, 0)
            column = lax.broadcasted_iota(jnp.int32, piece.shape, 1)
            ahead = (block - query_block) * rows - start % rows
            pieces.append(jnp.where(column + ahead <= row, piece, NEG_LARGE))
        return jnp.concatenate(pieces, axis=1)

    def run_group(group, first):
        keys = jnp.concatenate([ref[group, 0] for ref in key_refs], axis=0)
        values = jnp.concatenate([ref[group, 0] for ref in value_refs], axis=0)
        values = jnp.concatenate([values, ones], axis=1)

        def scores_of(start):
            return lax.dot_general(
                both_ref[start : start + step_rows],
                keys,
                (((1,), (1,)), ((), ())),
                preferred_element_type=jnp.float32,
            )

        coming = scores_of(0)
        for start in range(0, 2 * rows, step_rows):
            scores = coming * scale
            if start + step_rows < 2 * rows:
                coming = scores_of(start + step_rows)
            here = slice(start, start + step_rows)
            if first:
                scores = masked(scores, start, group)
            new_max = jnp.max(scores, axis=1, keepdims=True)
            if not first:
                old_max = max_ref[here, :1]
                new_max = jnp.maximum(old_max, new_max)
            expo = jnp.exp2(scores - new_max).astype(jnp.bfloat16)
            weighted = jnp.dot(expo, values, preferred_element_type=jnp.float32)
            if not first:
                weighted = weighted + acc_ref[here] * jnp.exp2(old_max - new_max)
            max_ref[here] = jnp.broadcast_to(new_max, (step_rows, max_ref.shape[1]))
            acc_ref[here] = weighted

    last = query_block // parts
    run_group(last, True)

    def step(group, carry):
        run_group(group, False)
        return carry

    lax.fori_loop(0, last, step, 0)
    head_mix = (
        acc_ref[:rows, :value_dim] / acc_ref[:rows, value_dim:]
        - lam_ref[pl.program_id(0)]
        * acc_ref[rows:, :value_dim]
        / acc_ref[rows:, value_dim:]
    )
    mean_sq = jnp.mean(head_mix * head_mix, axis=1, keepdims=True)
    normed = head_mix * lax.rsqrt(mean_sq + EPSILON) * gain_ref[...]
    out_ref[0, 0] = normed.astype(jnp.bfloat16)


def attend(place, lam, gain, queries, keys, values, inner, head_dim):
    spread, heads, rows, pair = queries.shape
    value_dim = values[0].shape[3]
    smem = pl.BlockSpec(memory_space=pltpu.SMEM)

    def whole_head(array):
        blocks, _, length, width = array.shape
        return pl.BlockSpec((blocks, 1, length, width), lambda h, j: (0, h, 0, 0))

    return pl.pallas_call(
        functools.partial(
            attention_kernel, inner=inner, head_dim=head_dim, parts=len(keys)
        ),
        grid=(heads, spread),
        in_specs=[
            smem,
            smem,
            pl.BlockSpec((1, value_dim), lambda h, j: (0, 0)),
            pl.BlockSpec((1, 1, rows, pair), lambda h, j: (j, h, 0, 0)),
            *[whole_head(array) for array in (*keys, *values)],
        ],
        out_specs=pl.BlockSpec((1, 1, rows, value_dim), lambda h, j: (j, h, 0, 0)),
        out_shape=jax.ShapeDtypeStruct((spread, heads, rows, value_dim), jnp.bfloat16),
        scratch_shapes=[
            pltpu.VMEM((2 * rows, pair), jnp.bfloat16),
            pltpu.VMEM((2 * rows, 128), jnp.float32),
            pltpu.VMEM((2 * rows, 2 * value_dim), jnp.float32),
        ],
        compiler_params=pltpu.CompilerParams(
            dimension_semantics=("arbitrary", "arbitrary"), vmem_limit_bytes=56 << 20
        ),
        cost_estimate=pl.CostEstimate(
            flops=spread * heads * rows * rows * inner * spread * 1024,
            transcendentals=spread * heads * rows * rows * inner * spread,
            bytes_accessed=sum(array.size * 2 for array in (*keys, *values)),
        ),
        name="diff_attention",
    )(place, lam, gain, queries, *keys, *values)


def exchanged(blocks, groups):
    return lax.all_to_all(
        blocks, "sp", split_axis=0, concat_axis=0, tiled=True, axis_index_groups=groups
    )


def mirrored(block, bit):
    return lax.ppermute(block, "sp", [(i, i ^ bit) for i in range(lax.axis_size("sp"))])


def from_beside(block, inner, spread, groups):
    if inner & (inner - 1) == 0 and inner <= 4:
        held = [block]
        bit = inner // 2
        while bit > 0:
            held = held + [mirrored(piece, bit) for piece in held]
            bit //= 2
        width = inner.bit_length() - 1
        order = [int(format(t, "b").zfill(width)[::-1], 2) if width else 0 for t in range(inner)]
        return [held[order[t]] for t in range(inner)]
    full = lax.all_gather(block, "sp", axis=0, axis_index_groups=groups)
    return [jnp.swapaxes(full, 0, 1).reshape(inner * spread, *block.shape[1:])]


def local(
    tokens,
    pre_gain,
    w_query,
    w_key,
    w_value,
    w_pool,
    lambdas,
    sub_gain,
    group_weight,
    pool_scale,
    w_out,
):
    tok_rows = tokens.shape[0]
    model_width = tokens.shape[1] * lax.axis_size("tp")
    local_heads = lambdas.shape[0]
    head_dim = w_query.shape[1] // (2 * local_heads)
    value_dim = w_value.shape[1] // local_heads
    local_groups = group_weight.shape[0]
    group_dim = group_weight.shape[1]
    q_cols = w_query.shape[1]
    v_cols = w_value.shape[1]
    sp_size = lax.axis_size("sp")
    tp_size = lax.axis_size("tp")
    spread = math.gcd(local_heads, sp_size)
    inner = sp_size // spread
    heads_here = local_heads // spread
    apart = [[r + inner * j for j in range(spread)] for r in range(inner)]
    beside = [[r + inner * j for r in range(inner)] for j in range(spread)]
    my_sp = lax.axis_index("sp")
    my_tp = lax.axis_index("tp")
    w_cat = jnp.concatenate([w_query, w_key, w_value, w_pool], axis=1)
    w_in_full = lax.all_gather(w_cat, "sp", axis=0, tiled=True)
    w_out_t = lax.all_gather(w_out.T, "sp", axis=0, tiled=True)
    gain_row = pre_gain.reshape(1, -1)
    if tp_size == 2:
        other = swapped(tokens, "tp")
        pieces = jnp.where(
            my_tp == 0,
            jnp.concatenate([tokens, other], axis=1),
            jnp.concatenate([other, tokens], axis=1),
        )
    else:
        pieces = lax.all_gather(tokens, "tp", axis=1, tiled=True)
    gains = lax.all_gather(gain_row, "tp", axis=1, tiled=True)
    feature_part = pieces.astype(jnp.float32)
    scaled = (feature_part * gains.astype(jnp.float32)).astype(jnp.bfloat16)
    squares = jnp.sum(feature_part * feature_part, axis=1)
    inverse = lax.rsqrt(squares / model_width + EPSILON)
    projection = jnp.dot(scaled, w_in_full, preferred_element_type=jnp.float32)
    projected = (projection * inverse[:, None]).astype(jnp.bfloat16)
    pair = 2 * head_dim

    def by_head(first, width):
        return jnp.stack(
            [projected[:, first + h * width : first + (h + 1) * width] for h in range(local_heads)]
        )

    keys = by_head(q_cols, pair)
    values = by_head(2 * q_cols, value_dim)
    queries = by_head(0, pair)
    pool_in = projected[:, 2 * q_cols + v_cols :]
    positions = my_sp * tok_rows + jnp.arange(tok_rows, dtype=jnp.int32)
    if spread > 1:
        keys = exchanged(keys, apart)
        values = exchanged(values, apart)
        queries = exchanged(queries, apart)
    shape = (spread, heads_here, tok_rows)
    keys = from_beside(keys.reshape(*shape, pair), inner, spread, beside)
    values = from_beside(values.reshape(*shape, value_dim), inner, spread, beside)
    queries = queries.reshape(*shape, pair)
    lam = lax.dynamic_slice_in_dim(lambdas, (my_sp // inner) * heads_here, heads_here)
    place = (my_sp % inner).astype(jnp.int32).reshape(1)
    attention = attend(
        place, lam, sub_gain.reshape(1, -1), queries, keys, values, inner, head_dim
    )
    attention = attention.reshape(local_heads, tok_rows, value_dim)
    if spread > 1:
        attention = exchanged(attention, apart)
    attention = jnp.transpose(attention, (1, 0, 2))
    halo_rows = passed_along(pool_in[tok_rows - RIM_ROWS :], "sp", 1)
    extended = jnp.concatenate([halo_rows, pool_in], axis=0).astype(jnp.float32)
    running = jnp.concatenate(
        [jnp.zeros((1, extended.shape[1]), jnp.float32), jnp.cumsum(extended, axis=0)], axis=0
    )
    running_top = running[RIM_ROWS + 1 :]
    window_ids = (
        lax.axis_index("tp") * local_groups + jnp.arange(local_groups, dtype=jnp.int32)
    ) % len(WINDOWS)
    column_window = jnp.repeat(window_ids, group_dim)
    average = jnp.zeros_like(running_top)
    for window_slot, window_span in enumerate(WINDOWS):
        running_low = running[RIM_ROWS + 1 - window_span : RIM_ROWS + 1 - window_span + tok_rows]
        window_count = jnp.minimum(positions + 1, window_span).astype(jnp.float32)
        average = average + jnp.where(
            column_window[None, :] == window_slot,
            (running_top - running_low) / window_count[:, None],
            0.0,
        )
    differ = (
        (average - pool_in.astype(jnp.float32))
        .astype(jnp.bfloat16)
        .reshape(tok_rows, local_groups, group_dim)
    )
    pooled = jnp.einsum("tgc,gcd->tgd", differ, group_weight, preferred_element_type=jnp.float32)
    pooled = (pooled * pool_scale.reshape(local_groups, group_dim)).astype(jnp.bfloat16)
    branch = jnp.concatenate([attention, pooled], axis=2).reshape(tok_rows, -1)

    def out_of(rows):
        return lax.dot_general(
            rows, w_out_t, (((1,), (1,)), ((), ())), preferred_element_type=jnp.float32
        )

    if tp_size == 2:
        half = tok_rows // 2
        sent = out_of(lax.dynamic_slice_in_dim(branch, (1 - my_tp) * half, half))
        arrived = swapped(sent.astype(jnp.bfloat16), "tp")
        kept = lax.optimization_barrier(
            out_of(lax.dynamic_slice_in_dim(branch, my_tp * half, half))
        )
        return (kept + arrived.astype(jnp.float32)).astype(jnp.bfloat16)
    return lax.psum_scatter(
        out_of(branch).astype(jnp.bfloat16), "tp", scatter_dimension=0, tiled=True
    )


def solution(mesh):
    placed = (
        P("sp", "tp"),
        P("tp"),
        P("sp", "tp"),
        P("sp", "tp"),
        P("sp", "tp"),
        P("sp", "tp"),
        P("tp"),
        P(),
        P("tp", None, None),
        P("tp"),
        P("tp", "sp"),
    )
    return jax.shard_map(
        local, mesh=mesh, in_specs=placed, out_specs=P(("sp", "tp"), None), check_vma=False
    )
```
